32 devices in a mesh: ep: 8 (over z, y), tp: 4 (over x, core).
Axes of the slice: x: 2, y: 2, z: 4, core: 2. Of those that a mesh axis runs over, the one named last changes fastest.
Arguments:
- tokens: bfloat16 [2560, 2048], P('ep'), may hold values from -12 to 12, as said below
- cotangent: bfloat16 [2560, 2048], P('ep'), may hold values from -0.59765625 to 0.59765625
- route_ids: int32 [2560, 2], P('ep'), may hold values from 0 to 7, all different within a row; in each aligned block of 320 rows (0 to 319, 320 to 639, ...) at most 160 rows name the same one
- route_weights: bfloat16 [2560, 2], P('ep'), may hold values from 0.049804688 to 1
- w_gate: bfloat16 [8, 2048, 2048], P('ep', None, 'tp'), may hold values from -0.125 to 0.125
- w_up: bfloat16 [8, 2048, 2048], P('ep', None, 'tp'), may hold values from -0.125 to 0.125
- w_down: bfloat16 [8, 2048, 2048], P('ep', 'tp'), may hold values from -0.125 to 0.125
- dense_in: bfloat16 [2048, 256], P(('ep', 'tp')), may hold values from -0.125 to 0.125
- dense_out: bfloat16 [2048, 256], P(('ep', 'tp')), may hold values from -0.375 to 0.375
- dense_gate: bfloat16 [2048], replicated, may hold values from -0.125 to 0.125
Outputs:
- grad_tokens: bfloat16 [2560, 2048], P('ep', 'tp')
- grad_route_weights: bfloat16 [2560, 2], P('ep')
- grad_gate: float32 [8, 2048, 2048], P('ep', None, 'tp')
- grad_up: float32 [8, 2048, 2048], P('ep', None, 'tp')
- grad_down: float32 [8, 2048, 2048], P('ep', 'tp')
- grad_dense_in: float32 [2048, 256], P(('ep', 'tp'))
- grad_dense_out: float32 [2048, 256], P(('ep', 'tp'))
- grad_dense_gate: float32 [2048], P(('ep', 'tp'))
The draws below stay inside these ranges and needn't reach their ends.
Inputs may be any that keep to these rules, and one draw needn't show every extreme that they name: `route_ids`: each row names 2 different experts; among the rows of one index of ep no expert is named more than 160 times, and that count is reached. `tokens`: rows carry scales between 0.5 and 2 that differ from row to row.
All inputs are finite; a program needn't handle non-finite values.
Results may differ from the reference program's by a relative error of at most 0.01.
Values may be sent and summed in bfloat16 or wider, within the bound.
A program may use at most 128 MiB of HBM per device.

```python
import math
import jax
import jax.numpy as jnp
import numpy as np
from jax import lax

D = 2048
FF = 2048
R = 256
TOP = 2
TOK_DEV = 320
EXPERTS = 8
CAP = 160
TOKENS = 2560
N_EP = 8
N_TP = 4


def draw_tokens(key, part):
    base_key = jax.random.fold_in(key, 11)
    scale_key = jax.random.fold_in(key, 12)
    scales = jnp.exp(jax.random.uniform(scale_key, (TOKENS, 1), jnp.float32, math.log(0.5), math.log(2.0)))
    base = jax.random.normal(base_key, (TOKENS, D), jnp.float32)
    base = jnp.clip(base, -6.0, 6.0)
    return (base * scales).astype(jnp.bfloat16)


def levels(own_key, extent, pieces, low, top_value):
    def one(dim, blocks):
        draws = jax.random.uniform(jax.random.fold_in(jax.random.fold_in(own_key, 6), dim), (blocks,), jnp.float32, low / len(pieces), top_value / len(pieces))
        return jnp.repeat(jnp.exp(draws), extent[dim] // blocks).reshape((-1,) + (1,) * (len(extent) - dim - 1))

    loudness = one(*pieces[0])
    for cut in pieces[1:]:
        loudness = loudness * one(*cut)
    return loudness


def routed_block(rng, own, number, rows, number_of, top, limit, slope):
    order = jax.random.permutation(rng, number_of)
    crowded, common = shares(number_of, rows * top, limit, slope, True), shares(number_of, rows * top, limit, slope, False)
    places = jnp.arange(number_of)

    def named(lengths, offset_by):
        used = int((lengths > 0).sum())
        fixed = max(1, used // 4)
        passed = fixed + (places - fixed + offset_by * (used - fixed)) % max(1, number_of - fixed)
        return jnp.zeros((number_of,), jnp.int32).at[order[jnp.where(places < fixed, places, passed)]].set(jnp.asarray(lengths, jnp.int32))

    lengths = jnp.where(number % 4 == 0, named(crowded, number // 4), named(common, number - number // 4 - 1))
    mixed = jax.random.permutation(jax.random.fold_in(own, 3), number_of)
    giver, receiver = mixed[0:number_of // 2 * 2:2], mixed[1:number_of // 2 * 2:2]
    margin = jnp.minimum(lengths[giver] - 1, limit - lengths[receiver]) // 2
    margin = jnp.where((giver == order[0]) | (receiver == order[0]) | (lengths[receiver] == 0), 0, jnp.maximum(margin, 0))
    passed = jax.random.randint(jax.random.fold_in(own, 4), (number_of // 2,), 0, 1 << 20) % (margin + 1)
    lengths = lengths.at[giver].add(-passed).at[receiver].add(passed)
    items = jnp.searchsorted(jnp.cumsum(lengths), jnp.arange(rows * top), side="right").astype(jnp.int32)
    grid = items.reshape(top, rows).T
    grid = grid[jax.random.permutation(jax.random.fold_in(own, 1), rows)]
    offset_by = jax.random.randint(jax.random.fold_in(own, 2), (rows, 1), 0, top)
    return jnp.take_along_axis(grid, (jnp.arange(top)[None, :] + offset_by) % top, axis=1)


def shares(amount, total, limit, skew, full):
    weights = [(1 << 20) // math.isqrt(rank ** skew) + 1 for rank in range(1, amount + 1)]
    largest = limit if full else min(limit, max(-(-total // amount), total * weights[0] // sum(weights)))
    least = 1 if total - largest >= amount - 1 else 0
    given, rest = [largest] + [least] * (amount - 1), total - largest - least * (amount - 1)
    while rest > 0:
        free = [i for i in range(1, amount) if given[i] < largest] or [i for i in range(1, amount) if given[i] < limit]
        whole, left = sum([weights[i] for i in free]), rest
        for i in free:
            extra = min(limit - given[i], max(1, left * weights[i] // whole), rest)
            given[i] = given[i] + extra
            rest = rest - extra
    return np.array(given)


def scatter_about(stream_key, shape, deviation, most, split=(), kind=jnp.bfloat16):
    values = jax.random.normal(stream_key, shape, jnp.float32) * deviation
    if len(split) > 0:
        values = levels(stream_key, shape, split, -0.22, 0.18) * values
    return jnp.clip(values, min=-most, max=most).astype(kind)


def setup_inputs(seed: int = 0) -> dict:
    keys = jax.random.split(jax.random.key(seed), 11)
    tokens = draw_tokens(jax.random.fold_in(keys[10], 71), 0)
    cotangent = scatter_about(keys[1], (TOKENS, D), 0.1, 0.59765625, ((0, 8),))
    route_ids_keys = jax.random.split(jax.random.fold_in(keys[2], 1), TOKENS // TOK_DEV)
    route_ids_turns = jax.random.permutation(jax.random.fold_in(keys[2], 3), TOKENS // TOK_DEV)
    route_ids = jax.vmap(lambda own, number: routed_block(jax.random.fold_in(keys[2], 2), own, number, TOK_DEV, EXPERTS, TOP, CAP, 2))(route_ids_keys, route_ids_turns).reshape((TOKENS, TOP))
    route_weights = jnp.clip(0.049804688 + 0.9501953 * jax.random.uniform(keys[3], (TOKENS, TOP), jnp.float32) ** levels(keys[3], (TOKENS, TOP), ((0, 8),), -0.2, 0.2), 0.049804688, 1.0).astype(jnp.bfloat16)
    w_gate = scatter_about(keys[4], (EXPERTS, D, FF), D ** -0.5, 0.125, ((0, 8), (2, 4)))
    w_up = scatter_about(keys[5], (EXPERTS, D, FF), D ** -0.5, 0.125, ((0, 8), (2, 4)))
    w_down = scatter_about(keys[6], (EXPERTS, FF, D), FF ** -0.5, 0.125, ((0, 8), (1, 4)))
    dense_in = scatter_about(keys[7], (D, R), D ** -0.5, 0.125, ((0, 32),))
    dense_out = scatter_about(keys[8], (D, R), R ** -0.5, 0.375, ((0, 32),))
    dense_gate = scatter_about(keys[9], (D,), D ** -0.5, 0.125)
    return dict(tokens=tokens, cotangent=cotangent, route_ids=route_ids, route_weights=route_weights, w_gate=w_gate, w_up=w_up, w_down=w_down, dense_in=dense_in, dense_out=dense_out, dense_gate=dense_gate)


CLAMP_LIMIT = 7.0
SIG_SLOPE = 1.702


def expert_grads(packed):
    x_rows, dy_rows, weight_rows, gate_w, up_w, down_w = packed
    gate_pre = jnp.dot(x_rows, gate_w, preferred_element_type=jnp.float32)
    up_pre = jnp.dot(x_rows, up_w, preferred_element_type=jnp.float32)
    gate_clamp = jnp.minimum(gate_pre, CLAMP_LIMIT)
    up_clamp = jnp.clip(up_pre, -CLAMP_LIMIT, CLAMP_LIMIT)
    sig = jax.nn.sigmoid(SIG_SLOPE * gate_clamp)
    act = (gate_clamp * sig * (up_clamp + 1.0)).astype(jnp.bfloat16)
    back = lax.dot_general(dy_rows, down_w, (((1,), (1,)), ((), ())), preferred_element_type=jnp.float32)
    weight_grad = jnp.sum(act.astype(jnp.float32) * back, axis=1).astype(jnp.bfloat16)
    route_col = weight_rows.astype(jnp.float32)[:, None]
    d_act = route_col * back
    d_gate = jnp.where(gate_pre < CLAMP_LIMIT, d_act * (up_clamp + 1.0) * (sig + SIG_SLOPE * gate_clamp * sig * (1.0 - sig)), 0.0).astype(jnp.bfloat16)
    d_up = jnp.where(jnp.abs(up_pre) < CLAMP_LIMIT, d_act * gate_clamp * sig, 0.0).astype(jnp.bfloat16)
    scaled_cot = (route_col * dy_rows.astype(jnp.float32)).astype(jnp.bfloat16)
    contract_rows = (((0,), (0,)), ((), ()))
    grad_gate = lax.dot_general(x_rows, d_gate, contract_rows, preferred_element_type=jnp.float32)
    grad_up = lax.dot_general(x_rows, d_up, contract_rows, preferred_element_type=jnp.float32)
    grad_down = lax.dot_general(act, scaled_cot, contract_rows, preferred_element_type=jnp.float32)
    slot_count, hidden = d_gate.shape
    model_width = gate_w.shape[0]
    group = hidden // N_TP
    partials = jnp.einsum('sjf,djf->jsd', d_gate.astype(jnp.float32).reshape(slot_count, N_TP, group), gate_w.astype(jnp.float32).reshape(model_width, N_TP, group))
    partials = partials + jnp.einsum('sjf,djf->jsd', d_up.astype(jnp.float32).reshape(slot_count, N_TP, group), up_w.astype(jnp.float32).reshape(model_width, N_TP, group))
    rounded = lax.optimization_barrier(partials.astype(jnp.bfloat16))
    row_grad = jnp.sum(rounded.astype(jnp.float32), axis=0).astype(jnp.bfloat16)
    return grad_gate, grad_up, grad_down, row_grad, weight_grad


def reference(tokens, cotangent, route_ids, route_weights, w_gate, w_up, w_down, dense_in, dense_out, dense_gate):
    total_tokens, model_width = tokens.shape
    top_k = route_ids.shape[1]
    expert_count = w_gate.shape[0]
    per_device = total_tokens // N_EP
    ids = route_ids.reshape(N_EP, per_device * top_k).astype(jnp.int32)
    one_hot = (ids[:, :, None] == jnp.arange(expert_count, dtype=jnp.int32)[None, None, :]).astype(jnp.int32)
    earlier = jnp.cumsum(one_hot, axis=1) - one_hot
    slot_index = jnp.sum(earlier * one_hot, axis=2)
    source_dev = jnp.arange(N_EP, dtype=jnp.int32)[:, None]
    position = (ids * (N_EP * CAP) + source_dev * CAP + slot_index).reshape(-1).astype(jnp.int32)
    token_of = (jnp.arange(total_tokens * top_k, dtype=jnp.int32) // top_k).astype(jnp.int32)
    slot_total = expert_count * N_EP * CAP
    x_buf = jnp.zeros((slot_total, model_width), jnp.bfloat16).at[position].set(tokens[token_of]).reshape(expert_count, N_EP * CAP, model_width)
    dy_buf = jnp.zeros((slot_total, model_width), jnp.bfloat16).at[position].set(cotangent[token_of]).reshape(expert_count, N_EP * CAP, model_width)
    weight_buf = jnp.zeros((slot_total,), jnp.bfloat16).at[position].set(route_weights.reshape(-1)).reshape(expert_count, N_EP * CAP)
    grad_gate, grad_up, grad_down, row_grad, weight_grad = lax.map(expert_grads, (x_buf, dy_buf, weight_buf, w_gate, w_up, w_down))
    expert_dx = row_grad.reshape(slot_total, model_width)[position].astype(jnp.float32).reshape(total_tokens, top_k, model_width)
    expert_dx = jnp.sum(expert_dx, axis=1)
    grad_route_weights = weight_grad.reshape(-1)[position].reshape(total_tokens, top_k)

    dense_pre = jnp.dot(tokens, dense_in, preferred_element_type=jnp.float32)
    dense_act = jax.nn.silu(dense_pre).astype(jnp.bfloat16)
    dense_val = lax.dot_general(dense_act, dense_out, (((1,), (1,)), ((), ())), preferred_element_type=jnp.float32)
    mix = jax.nn.sigmoid(jnp.dot(tokens, dense_gate, preferred_element_type=jnp.float32))
    cot_wide = cotangent.astype(jnp.float32)
    dense_scaled = (mix[:, None] * cot_wide).astype(jnp.bfloat16)
    dense_back = jnp.dot(dense_scaled, dense_out, preferred_element_type=jnp.float32)
    sig_pre = jax.nn.sigmoid(dense_pre)
    dense_dpre = (dense_back * sig_pre * (1.0 + dense_pre * (1.0 - sig_pre))).astype(jnp.bfloat16)
    dlogit = mix * (1.0 - mix) * jnp.sum(cot_wide * dense_val, axis=1)
    dense_dx = lax.dot_general(dense_dpre, dense_in, (((1,), (1,)), ((), ())), preferred_element_type=jnp.float32)
    dense_dx = dense_dx + dlogit[:, None] * dense_gate.astype(jnp.float32)[None, :]
    grad_tokens = (dense_dx + expert_dx).astype(jnp.bfloat16)
    contract_rows = (((0,), (0,)), ((), ()))
    grad_dense_in = lax.dot_general(tokens, dense_dpre, contract_rows, preferred_element_type=jnp.float32)
    grad_dense_out = lax.dot_general(dense_scaled, dense_act, contract_rows, preferred_element_type=jnp.float32)
    grad_dense_gate = jnp.sum(tokens.astype(jnp.float32) * dlogit[:, None], axis=0)
    return (grad_tokens, grad_route_weights, grad_gate, grad_up, grad_down, grad_dense_in, grad_dense_out, grad_dense_gate)
```

```python
import functools

import jax
import jax.numpy as jnp
from jax import lax
from jax.experimental import pallas as pl
from jax.experimental.pallas import tpu as pltpu
from jax.sharding import PartitionSpec as P

CLAMP_LIMIT = 7.0
SIG_SLOPE = 1.702
MESH = pl.DeviceIdType.MESH
ANY = pl.BlockSpec(memory_space=pl.ANY)
VMEM = pl.BlockSpec(memory_space=pltpu.VMEM)


def greet(devices):
    barrier = pltpu.get_barrier_semaphore()
    for device in devices:
        pl.semaphore_signal(barrier, inc=1, device_id=device, device_id_type=MESH)
    pl.semaphore_wait(barrier, len(devices))


def dispatch_kernel(
    n_ep,
    x_quarter,
    dy_quarter,
    x_own,
    dy_own,
    weight_rows,
    in_own,
    out_own,
    x_all,
    dy_all,
    weight_all,
    in_all,
    out_all,
    own_buf,
    shard_buf,
    local_sem,
    send_rows,
    recv_rows,
    send_shard,
    recv_shard,
    send_w,
    recv_w,
):
    me = lax.axis_index("ep")
    t = lax.axis_index("tp")
    half = t // 2
    side = t % 2
    t_core = half * 2 + 1 - side
    t_x = (1 - half) * 2 + side
    cols = x_quarter.shape[2]

    def ahead(k):
        return lax.rem(me + k, n_ep)

    def behind(k):
        return lax.rem(me + n_ep - k, n_ep)

    core_peer = (me, t_core)
    x_peer = (me, t_x)
    greet([(ahead(k), t) for k in range(1, n_ep)] + [core_peer, x_peer])

    rows_in = (x_quarter, dy_quarter)
    rows_out = (x_all, dy_all)
    shards_in = (in_own, out_own)
    shards_out = (in_all, out_all)

    def row_slice(a, i, q):
        return rows_out[a].at[i, :, pl.ds(pl.multiple_of(q * cols, cols), cols)]

    def copy_to(src, dst, send, recv, device):
        return pltpu.make_async_remote_copy(
            src_ref=src,
            dst_ref=dst,
            send_sem=send,
            recv_sem=recv,
            device_id=device,
            device_id_type=MESH,
        )

    started = []

    def go(copy):
        copy.start()
        started.append(copy)
        return copy

    def shard_hop(a, kind, k, src_i, first=False):
        if kind == 0:
            return copy_to(
                shards_in[a],
                shards_out[a].at[me, t],
                send_shard.at[a, 0, k],
                recv_shard.at[a, 0, k],
                (ahead(k), t),
            )
        own = shards_in[a] if first else shards_out[a].at[src_i, t]
        if kind == 1:
            return copy_to(
                own,
                shards_out[a].at[src_i, t],
                send_shard.at[a, 1, k],
                recv_shard.at[a, 1, k],
                x_peer,
            )
        if kind == 2:
            return copy_to(
                own,
                shards_out[a].at[src_i, t],
                send_shard.at[a, 2, k],
                recv_shard.at[a, 2, k],
                core_peer,
            )
        return copy_to(
            shards_out[a].at[src_i, t_x],
            shards_out[a].at[src_i, t_x],
            send_shard.at[a, 3, k],
            recv_shard.at[a, 3, k],
            core_peer,
        )

    def row_hop(a, kind, k, i):
        if kind == 0:
            return copy_to(
                rows_in[a].at[ahead(k)],
                row_slice(a, me, t),
                send_rows.at[a, 0, k],
                recv_rows.at[a, 0, k],
                (ahead(k), t),
            )
        if kind == 3:
            return copy_to(
                row_slice(a, i, t_x),
                row_slice(a, i, t_x),
                send_rows.at[a, 3, k],
                recv_rows.at[a, 3, k],
                core_peer,
            )
        return copy_to(
            row_slice(a, i, t),
            row_slice(a, i, t),
            send_rows.at[a, kind, k],
            recv_rows.at[a, kind, k],
            x_peer if kind == 1 else core_peer,
        )

    def w_hop(k):
        return copy_to(
            weight_rows.at[ahead(k)],
            weight_all.at[me],
            send_w.at[k],
            recv_w.at[k],
            (ahead(k), t),
        )

    for a in range(2):
        go(shard_hop(a, 1, 0, me, True))
        go(shard_hop(a, 2, 0, me, True))
    for k in range(1, n_ep):
        for a in range(2):
            go(shard_hop(a, 0, k, me))
        go(w_hop(k))
        for a in range(2):
            go(row_hop(a, 0, k, me))

    ins = [
        pltpu.make_async_copy(x_own, own_buf.at[0], local_sem.at[0]),
        pltpu.make_async_copy(dy_own, own_buf.at[1], local_sem.at[1]),
        pltpu.make_async_copy(in_own, shard_buf.at[0], local_sem.at[2]),
        pltpu.make_async_copy(out_own, shard_buf.at[1], local_sem.at[3]),
    ]
    outs = [
        pltpu.make_async_copy(own_buf.at[0], x_all.at[me], local_sem.at[4]),
        pltpu.make_async_copy(own_buf.at[1], dy_all.at[me], local_sem.at[5]),
        pltpu.make_async_copy(shard_buf.at[0], in_all.at[me, t], local_sem.at[6]),
        pltpu.make_async_copy(shard_buf.at[1], out_all.at[me, t], local_sem.at[7]),
    ]
    for c in ins:
        c.start()
    weight_all[pl.ds(me, 1)] = weight_rows[pl.ds(me, 1)]
    for c, o in zip(ins, outs):
        c.wait()
        o.start()

    def relay(k):
        i = behind(k)
        for a in range(2):
            shard_hop(a, 1, k, i).wait_recv()
            go(shard_hop(a, 3, k, i))
            if k > 0:
                row_hop(a, 1, k, i).wait_recv()
                go(row_hop(a, 3, k, i))

    for k in range(1, n_ep):
        i = behind(k)
        for a in range(2):
            shard_hop(a, 0, k, i).wait_recv()
            go(shard_hop(a, 1, k, i))
            go(shard_hop(a, 2, k, i))
            row_hop(a, 0, k, i).wait_recv()
            go(row_hop(a, 1, k, i))
            go(row_hop(a, 2, k, i))
        relay(k - 1)
    relay(n_ep - 1)

    for k in range(n_ep):
        i = behind(k)
        for a in range(2):
            for kind in (2, 3):
                shard_hop(a, kind, k, i).wait_recv()
                if k > 0:
                    row_hop(a, kind, k, i).wait_recv()
        if k > 0:
            w_hop(k).wait_recv()
    for c in started:
        c.wait_send()
    for o in outs:
        o.wait()


def return_kernel(
    n_ep,
    n_tp,
    part,
    grad_in,
    grad_out,
    grad_gate,
    weight_part,
    rows_back,
    in_back,
    out_back,
    gate_back,
    weight_back,
    from_core,
    to_x,
    from_x,
    to_ep,
    send_core,
    recv_core,
    send_x,
    recv_x,
    send_ep,
    recv_ep,
    send_grad,
    recv_grad,
    send_w,
    recv_w,
):
    me = lax.axis_index("ep")
    t = lax.axis_index("tp")
    half = t // 2
    side = t % 2
    t_core = half * 2 + 1 - side
    t_x = (1 - half) * 2 + side
    cols = rows_back.shape[2]

    def ahead(k):
        return lax.rem(me + k, n_ep)

    def quarter(q):
        return pl.ds(pl.multiple_of(q * cols, cols), cols)

    core_peer = (me, t_core)
    x_peer = (me, t_x)
    others = [
        (ahead(k), lax.rem(t + d, n_tp))
        for k in range(n_ep)
        for d in range(n_tp)
        if k > 0 or d > 0
    ]
    greet(others)

    def copy_to(src, dst, send, recv, device):
        return pltpu.make_async_remote_copy(
            src_ref=src,
            dst_ref=dst,
            send_sem=send,
            recv_sem=recv,
            device_id=device,
            device_id_type=MESH,
        )

    started = []

    def go(copy):
        copy.start()
        started.append(copy)

    order = list(range(1, n_ep)) + [0]

    def core_hop(k, h):
        j = ahead(k)
        return copy_to(
            part.at[j, :, quarter(h * 2 + 1 - side)],
            from_core.at[k, h],
            send_core.at[k, h],
            recv_core.at[k, h],
            core_peer,
        )

    def x_hop(k):
        return copy_to(to_x.at[k], from_x.at[k], send_x.at[k], recv_x.at[k], x_peer)

    def ep_hop(k):
        return copy_to(
            to_ep.at[k], rows_back.at[me], send_ep.at[k], recv_ep.at[k], (ahead(k), t)
        )

    for k in order:
        for h in range(2):
            go(core_hop(k, h))
    grads = ((grad_in, in_back), (grad_out, out_back), (grad_gate, gate_back))

    def grad_hop(a, k):
        src, dst = grads[a]
        return copy_to(
            src.at[ahead(k)],
            dst.at[me],
            send_grad.at[a, k],
            recv_grad.at[a, k],
            (ahead(k), t),
        )

    def w_hop(k, d):
        return copy_to(
            weight_part.at[ahead(k)],
            weight_back.at[me, t],
            send_w.at[k, d],
            recv_w.at[k, d],
            (ahead(k), lax.rem(t + d, n_tp)),
        )

    for k in range(n_ep):
        for d in range(n_tp):
            if k > 0 or d > 0:
                go(w_hop(k, d))
        if k > 0:
            for a in range(3):
                go(grad_hop(a, k))
    for a in range(3):
        grads[a][1][pl.ds(me, 1)] = grads[a][0][pl.ds(me, 1)]
    weight_back[pl.ds(me, 1), pl.ds(t, 1)] = weight_part[pl.ds(me, 1)][:, None]

    def finish(k):
        j = ahead(k)
        x_hop(k).wait_recv()
        mine = part[j, :, quarter(t)].astype(jnp.float32)
        mine = mine + from_core[k, half].astype(jnp.float32)
        mine = (mine + from_x[k].astype(jnp.float32)).astype(jnp.bfloat16)
        if k > 0:
            to_ep[k] = mine
            go(ep_hop(k))
        else:
            rows_back[me] = mine

    lag = 2
    for n, k in enumerate(order):
        j = ahead(k)
        for h in range(2):
            core_hop(k, h).wait_recv()
        other = part[j, :, quarter(t_x)].astype(jnp.float32)
        other = other + from_core[k, 1 - half].astype(jnp.float32)
        to_x[k] = other.astype(jnp.bfloat16)
        go(x_hop(k))
        if n >= lag:
            finish(order[n - lag])
    for k in order[n_ep - lag :]:
        finish(k)

    for k in range(n_ep):
        if k > 0:
            ep_hop(k).wait_recv()
            for a in range(3):
                grad_hop(a, k).wait_recv()
        for d in range(n_tp):
            if k > 0 or d > 0:
                w_hop(k, d).wait_recv()
    for c in started:
        c.wait_send()


def dispatch(n_ep, n_tp, *args):
    x_quarter, dy_quarter, x_own, dy_own, weight_rows, in_own, out_own = args
    cap, cols = x_quarter.shape[1:]
    width = x_own.shape[1]
    bf = jnp.bfloat16
    dma = pltpu.SemaphoreType.DMA
    rows = jax.ShapeDtypeStruct((n_ep, cap, width), bf)
    shard = jax.ShapeDtypeStruct((n_ep, n_tp) + in_own.shape, bf)
    return pl.pallas_call(
        functools.partial(dispatch_kernel, n_ep),
        out_shape=(
            rows,
            rows,
            jax.ShapeDtypeStruct(weight_rows.shape, weight_rows.dtype),
            shard,
            shard,
        ),
        in_specs=[ANY, ANY, ANY, ANY, VMEM, ANY, ANY],
        out_specs=(ANY, ANY, VMEM, ANY, ANY),
        scratch_shapes=[
            pltpu.VMEM((2, cap, width), bf),
            pltpu.VMEM((2,) + in_own.shape, bf),
            dma((8,)),
            dma((2, 4, n_ep)),
            dma((2, 4, n_ep)),
            dma((2, 4, n_ep)),
            dma((2, 4, n_ep)),
            dma((n_ep,)),
            dma((n_ep,)),
        ],
        compiler_params=pltpu.CompilerParams(collective_id=0, has_side_effects=True),
        name="dispatch",
    )(*args)


def give_back(n_ep, n_tp, *args):
    part, grad_in, grad_out, grad_gate, weight_part = args
    cap, width = part.shape[1:]
    cols = width // n_tp
    bf = jnp.bfloat16
    dma = pltpu.SemaphoreType.DMA
    same = lambda a: jax.ShapeDtypeStruct(a.shape, a.dtype)
    return pl.pallas_call(
        functools.partial(return_kernel, n_ep, n_tp),
        out_shape=(
            jax.ShapeDtypeStruct((n_ep, cap, cols), bf),
            same(grad_in),
            same(grad_out),
            same(grad_gate),
            jax.ShapeDtypeStruct((n_ep, n_tp) + weight_part.shape[1:], weight_part.dtype),
        ),
        in_specs=[VMEM] * 5,
        out_specs=(VMEM,) * 5,
        scratch_shapes=[
            pltpu.VMEM((n_ep, 2, cap, cols), bf),
            pltpu.VMEM((n_ep, cap, cols), bf),
            pltpu.VMEM((n_ep, cap, cols), bf),
            pltpu.VMEM((n_ep, cap, cols), bf),
            dma((n_ep, 2)),
            dma((n_ep, 2)),
            dma((n_ep,)),
            dma((n_ep,)),
            dma((n_ep,)),
            dma((n_ep,)),
            dma((3, n_ep)),
            dma((3, n_ep)),
            dma((n_ep, n_tp)),
            dma((n_ep, n_tp)),
        ],
        compiler_params=pltpu.CompilerParams(
            collective_id=1, has_side_effects=True, vmem_limit_bytes=40 * 1024 * 1024
        ),
        name="give_back",
    )(*args)


def shards(
    tokens,
    cotangent,
    route_ids,
    route_weights,
    w_gate,
    w_up,
    w_down,
    dense_in,
    dense_out,
    dense_gate,
):
    count_ep = lax.axis_size("ep")
    count_tp = lax.axis_size("tp")
    ep_index = lax.axis_index("ep")
    tp_index = lax.axis_index("tp")
    tok_dev, model_width = tokens.shape
    top_k = route_ids.shape[1]
    col_count = model_width // count_tp
    capacity = 2 * tok_dev * top_k // count_ep
    lanes = -(-capacity // 128) * 128
    slot_total = count_ep * capacity
    bf = jnp.bfloat16
    f32 = jnp.float32

    names = jnp.arange(count_ep, dtype=jnp.int32)
    chosen = route_ids[:, :, None] == names[None, None, :]
    member = jnp.any(chosen, axis=1).astype(bf)
    row = jnp.arange(tok_dev, dtype=jnp.int32)
    below = (row[None, :] < row[:, None]).astype(bf)
    rank = jnp.dot(below, member, preferred_element_type=f32)
    slot_index = jnp.sum(jnp.where(chosen, rank[:, None, :], 0.0), axis=2).astype(jnp.int32)
    target = route_ids * capacity + slot_index
    lane_target = route_ids * lanes + slot_index
    slots = jnp.arange(slot_total, dtype=jnp.int32)
    pick = slots[:, None] == target[:, 0][None, :]
    for k in range(1, top_k):
        pick = pick | (slots[:, None] == target[:, k][None, :])
    pick = pick.astype(bf)
    tok_part = lax.dynamic_slice_in_dim(tokens, tp_index * col_count, col_count, 1)
    cot_part = lax.dynamic_slice_in_dim(cotangent, tp_index * col_count, col_count, 1)
    quarter_shape = (count_ep, capacity, col_count)
    x_quarter = jnp.dot(pick, tok_part, preferred_element_type=bf).reshape(quarter_shape)
    dy_quarter = jnp.dot(pick, cot_part, preferred_element_type=bf).reshape(quarter_shape)
    pick_own = lax.dynamic_slice_in_dim(pick, ep_index * capacity, capacity, 0)
    x_own = jnp.dot(pick_own, tokens, preferred_element_type=bf)
    dy_own = jnp.dot(pick_own, cotangent, preferred_element_type=bf)
    lane_slots = jnp.arange(count_ep * lanes, dtype=jnp.int32)
    lane_hits = lane_target[:, :, None] == lane_slots[None, None, :]
    weight_rows = jnp.sum(
        jnp.where(lane_hits, route_weights.astype(f32)[:, :, None], 0.0), axis=(0, 1)
    ).astype(bf)
    weight_rows = jnp.broadcast_to(
        weight_rows.reshape(count_ep, 1, lanes), (count_ep, 16, lanes)
    )
    x_in, dy_in, weight_in, in_all, out_all = dispatch(
        count_ep, count_tp, x_quarter, dy_quarter, x_own, dy_own, weight_rows, dense_in, dense_out
    )
    in_whole = in_all.reshape(model_width, -1)
    out_whole = out_all.reshape(model_width, -1)

    x_slots = x_in.reshape(slot_total, model_width)
    dy_slots = dy_in.reshape(slot_total, model_width)
    route_col = weight_in[:, 0, :capacity].reshape(slot_total, 1).astype(f32)
    gate_w = w_gate[0]
    up_w = w_up[0]
    down_w = w_down[0]
    gate_pre = jnp.dot(x_slots, gate_w, preferred_element_type=f32)
    up_pre = jnp.dot(x_slots, up_w, preferred_element_type=f32)
    gate_clamp = jnp.minimum(gate_pre, CLAMP_LIMIT)
    up_clamp = jnp.clip(up_pre, -CLAMP_LIMIT, CLAMP_LIMIT)
    sig = jax.nn.sigmoid(SIG_SLOPE * gate_clamp)
    act = (gate_clamp * sig * (up_clamp + 1.0)).astype(bf)
    back = lax.dot_general(
        dy_slots, down_w, (((1,), (1,)), ((), ())), preferred_element_type=f32
    )
    d_act = route_col * back
    d_gate = jnp.where(
        gate_pre < CLAMP_LIMIT,
        d_act * (up_clamp + 1.0) * (sig + SIG_SLOPE * gate_clamp * sig * (1.0 - sig)),
        0.0,
    ).astype(bf)
    d_up = jnp.where(jnp.abs(up_pre) < CLAMP_LIMIT, d_act * gate_clamp * sig, 0.0).astype(bf)
    scaled_cot = (route_col * dy_slots.astype(f32)).astype(bf)
    contract_rows = (((0,), (0,)), ((), ()))
    grad_gate = lax.dot_general(x_slots, d_gate, contract_rows, preferred_element_type=f32)
    grad_up = lax.dot_general(x_slots, d_up, contract_rows, preferred_element_type=f32)
    grad_down = lax.dot_general(act, scaled_cot, contract_rows, preferred_element_type=f32)
    contract_cols = (((1,), (1,)), ((), ()))
    row_partial = lax.dot_general(d_gate, gate_w, contract_cols, preferred_element_type=f32)
    row_partial = row_partial + lax.dot_general(
        d_up, up_w, contract_cols, preferred_element_type=f32
    )
    part = row_partial.astype(bf).reshape(count_ep, capacity, model_width)
    weight_part = jnp.sum(act.astype(f32) * back, axis=1).reshape(count_ep, capacity)
    weight_part = jnp.pad(weight_part, ((0, 0), (0, lanes - capacity)))
    weight_part = jnp.broadcast_to(weight_part[:, None, :], (count_ep, 8, lanes))

    dense_pre = jnp.dot(tokens, in_whole, preferred_element_type=f32)
    dense_act = jax.nn.silu(dense_pre).astype(bf)
    dense_val = lax.dot_general(dense_act, out_whole, contract_cols, preferred_element_type=f32)
    mix = jax.nn.sigmoid(jnp.dot(tokens, dense_gate, preferred_element_type=f32))
    cot_wide = cotangent.astype(f32)
    dense_scaled = (mix[:, None] * cot_wide).astype(bf)
    dense_back = jnp.dot(dense_scaled, out_whole, preferred_element_type=f32)
    sig_pre = jax.nn.sigmoid(dense_pre)
    dense_dpre = (dense_back * sig_pre * (1.0 + dense_pre * (1.0 - sig_pre))).astype(bf)
    dlogit = mix * (1.0 - mix) * jnp.sum(cot_wide * dense_val, axis=1)
    in_rows = lax.dynamic_slice_in_dim(in_whole, tp_index * col_count, col_count, 0)
    gate_cols = lax.dynamic_slice_in_dim(dense_gate, tp_index * col_count, col_count, 0)
    dense_dx = lax.dot_general(dense_dpre, in_rows, contract_cols, preferred_element_type=f32)
    dense_dx = dense_dx + dlogit[:, None] * gate_cols.astype(f32)[None, :]
    block_cols = model_width // (count_ep * count_tp)
    tokens_own = lax.dynamic_index_in_dim(
        tokens.reshape(tok_dev, count_ep, count_tp, block_cols), tp_index, 2, keepdims=False
    ).reshape(tok_dev, count_ep * block_cols)
    scaled_own = lax.dynamic_index_in_dim(
        dense_scaled.reshape(tok_dev, count_ep, count_tp, block_cols), tp_index, 2, keepdims=False
    ).reshape(tok_dev, count_ep * block_cols)
    in_partial = lax.dot_general(tokens_own, dense_dpre, contract_rows, preferred_element_type=f32)
    out_partial = lax.dot_general(scaled_own, dense_act, contract_rows, preferred_element_type=f32)
    gate_partial = jnp.sum(tokens_own.astype(f32) * dlogit[:, None], axis=0)
    gate_partial = jnp.pad(
        gate_partial.reshape(count_ep, 1, block_cols), ((0, 0), (0, 7), (0, -block_cols % 128))
    )

    rows_back, in_back, out_back, gate_back, weight_back = give_back(
        count_ep,
        count_tp,
        part,
        in_partial.reshape(count_ep, block_cols, -1),
        out_partial.reshape(count_ep, block_cols, -1),
        gate_partial,
        weight_part,
    )
    grad_dense_in = jnp.sum(in_back, axis=0)
    grad_dense_out = jnp.sum(out_back, axis=0)
    grad_dense_gate = jnp.sum(gate_back[:, 0, :block_cols], axis=0)
    expert_dx = lax.dot_general(
        pick, rows_back.reshape(slot_total, col_count), contract_rows, preferred_element_type=f32
    )
    grad_tokens = (dense_dx + expert_dx).astype(bf)
    weight_grad = jnp.sum(weight_back[:, :, 0, :], axis=1).reshape(-1)
    grad_route_weights = jnp.sum(
        jnp.where(lane_hits, weight_grad[None, None, :], 0.0), axis=2
    ).astype(bf)
    return (
        grad_tokens,
        grad_route_weights,
        grad_gate[None],
        grad_up[None],
        grad_down[None],
        grad_dense_in,
        grad_dense_out,
        grad_dense_gate,
    )


def solution(mesh):
    placed = (
        P("ep", None),
        P("ep", None),
        P("ep", None),
        P("ep", None),
        P("ep", None, "tp"),
        P("ep", None, "tp"),
        P("ep", "tp", None),
        P(("ep", "tp"), None),
        P(("ep", "tp"), None),
        P(),
    )
    return jax.shard_map(
        shards,
        mesh=mesh,
        in_specs=placed,
        out_specs=(
            P("ep", "tp"),
            P("ep", None),
            P("ep", None, "tp"),
            P("ep", None, "tp"),
            P("ep", "tp", None),
            P(("ep", "tp"), None),
            P(("ep", "tp"), None),
            P(("ep", "tp")),
        ),
        check_vma=False,
    )
```

```python
import functools

import jax
import jax.numpy as jnp
from jax import lax
from jax.experimental import pallas as pl
from jax.experimental.pallas import tpu as pltpu
from jax.sharding import PartitionSpec as P

CLAMP_LIMIT = 7.0
SIG_SLOPE = 1.702
MESH = pl.DeviceIdType.MESH
ANY = pl.BlockSpec(memory_space=pl.ANY)
VMEM = pl.BlockSpec(memory_space=pltpu.VMEM)


def greet(devices):
    barrier = pltpu.get_barrier_semaphore()
    for device in devices:
        pl.semaphore_signal(barrier, inc=1, device_id=device, device_id_type=MESH)
    pl.semaphore_wait(barrier, len(devices))


def dispatch_kernel(
    n_ep,
    x_quarter,
    dy_quarter,
    x_own,
    dy_own,
    weight_rows,
    in_own,
    out_own,
    gate_w,
    up_w,
    down_w,
    x_all,
    scaled_all,
    act_all,
    dgate_all,
    dup_all,
    part_all,
    weight_part,
    in_all,
    out_all,
    dy_all,
    weight_all,
    shard_buf,
    local_sem,
    send_rows,
    recv_rows,
    send_shard,
    recv_shard,
    send_w,
    recv_w,
):
    me = lax.axis_index("ep")
    t = lax.axis_index("tp")
    half = t // 2
    side = t % 2
    t_core = half * 2 + 1 - side
    t_x = (1 - half) * 2 + side
    cap, cols = x_quarter.shape[1:]
    lanes = weight_rows.shape[2]
    f32 = jnp.float32
    bf = jnp.bfloat16

    def ahead(k):
        return lax.rem(me + k, n_ep)

    def behind(k):
        return lax.rem(me + n_ep - k, n_ep)

    core_peer = (me, t_core)
    x_peer = (me, t_x)
    greet([(ahead(k), t) for k in range(1, n_ep)] + [core_peer, x_peer])

    rows_in = (x_quarter, dy_quarter)
    rows_out = (x_all, dy_all)
    shards_in = (in_own, out_own)
    shards_out = (in_all, out_all)

    def row_slice(a, i, q):
        return rows_out[a].at[i, :, pl.ds(pl.multiple_of(q * cols, cols), cols)]

    def copy_to(src, dst, send, recv, device):
        return pltpu.make_async_remote_copy(
            src_ref=src,
            dst_ref=dst,
            send_sem=send,
            recv_sem=recv,
            device_id=device,
            device_id_type=MESH,
        )

    def shard_hop(a, kind, k, first=False):
        i = behind(k)
        sems = (send_shard.at[a, kind, k], recv_shard.at[a, kind, k])
        if kind == 0:
            return copy_to(shards_in[a], shards_out[a].at[me, t], *sems, (ahead(k), t))
        if kind == 3:
            block = shards_out[a].at[i, t_x]
            return copy_to(block, block, *sems, core_peer)
        block = shards_out[a].at[i, t]
        return copy_to(
            shards_in[a] if first else block, block, *sems, x_peer if kind == 1 else core_peer
        )

    def row_hop(a, kind, k):
        i = behind(k)
        sems = (send_rows.at[a, kind, k], recv_rows.at[a, kind, k])
        if kind == 0:
            return copy_to(rows_in[a].at[ahead(k)], row_slice(a, me, t), *sems, (ahead(k), t))
        block = row_slice(a, i, t_x if kind == 3 else t)
        return copy_to(block, block, *sems, x_peer if kind == 1 else core_peer)

    def w_hop(k):
        return copy_to(
            weight_rows.at[ahead(k)], weight_all.at[me], send_w.at[k], recv_w.at[k], (ahead(k), t)
        )

    for a in range(2):
        shard_hop(a, 1, 0, True).start()
        shard_hop(a, 2, 0, True).start()

    @pl.loop(1, n_ep)
    def _(k):
        for a in range(2):
            shard_hop(a, 0, k).start()
        w_hop(k).start()
        for a in range(2):
            row_hop(a, 0, k).start()

    ins = [
        pltpu.make_async_copy(in_own, shard_buf.at[0], local_sem.at[0]),
        pltpu.make_async_copy(out_own, shard_buf.at[1], local_sem.at[1]),
        pltpu.make_async_copy(x_own, x_all.at[me], local_sem.at[2]),
        pltpu.make_async_copy(dy_own, dy_all.at[me], local_sem.at[3]),
    ]
    outs = [
        pltpu.make_async_copy(shard_buf.at[0], in_all.at[me, t], local_sem.at[4]),
        pltpu.make_async_copy(shard_buf.at[1], out_all.at[me, t], local_sem.at[5]),
    ]
    for c in ins:
        c.start()
    weight_all[pl.ds(me, 1)] = weight_rows[pl.ds(me, 1)]
    for c in ins:
        c.wait()
    for c in outs:
        c.start()

    diagonal = lax.broadcasted_iota(jnp.int32, (cap, lanes), 0) == lax.broadcasted_iota(
        jnp.int32, (cap, lanes), 1
    )
    contract_cols = (((1,), (1,)), ((), ()))

    def compute(i):
        weight_row = weight_all[i, 0:1].astype(f32)
        route_col = jnp.sum(jnp.where(diagonal, weight_row, 0.0), axis=1, keepdims=True)
        x_rows = x_all[i]
        gate_pre = jnp.dot(x_rows, gate_w[...], preferred_element_type=f32)
        up_pre = jnp.dot(x_rows, up_w[...], preferred_element_type=f32)
        gate_clamp = jnp.minimum(gate_pre, CLAMP_LIMIT)
        up_clamp = jnp.clip(up_pre, -CLAMP_LIMIT, CLAMP_LIMIT)
        sig = jax.nn.sigmoid(SIG_SLOPE * gate_clamp)
        act = (gate_clamp * sig * (up_clamp + 1.0)).astype(bf)
        act_all[i] = act
        dy_rows = dy_all[i]
        scaled_all[i] = (route_col * dy_rows.astype(f32)).astype(bf)
        back = lax.dot_general(
            dy_rows, down_w[...], contract_cols, preferred_element_type=f32
        )
        weight_sum = jnp.sum(act.astype(f32) * back, axis=1, keepdims=True)
        weight_lane = jnp.sum(jnp.where(diagonal, weight_sum, 0.0), axis=0, keepdims=True)
        weight_part[i] = jnp.broadcast_to(weight_lane, (8, lanes))
        d_act = route_col * back
        d_gate = jnp.where(
            gate_pre < CLAMP_LIMIT,
            d_act * (up_clamp + 1.0) * (sig + SIG_SLOPE * gate_clamp * sig * (1.0 - sig)),
            0.0,
        ).astype(bf)
        d_up = jnp.where(jnp.abs(up_pre) < CLAMP_LIMIT, d_act * gate_clamp * sig, 0.0).astype(bf)
        dgate_all[i] = d_gate
        dup_all[i] = d_up
        part = lax.dot_general(d_gate, gate_w[...], contract_cols, preferred_element_type=f32)
        part = part + lax.dot_general(d_up, up_w[...], contract_cols, preferred_element_type=f32)
        part_all[i] = part.astype(bf)

    @pl.loop(0, n_ep + 2)
    def _(n):
        @pl.when((n >= 1) & (n < n_ep))
        def _():
            for a in range(2):
                shard_hop(a, 0, n).wait_recv()
                shard_hop(a, 1, n).start()
                shard_hop(a, 2, n).start()
            for a in range(2):
                row_hop(a, 0, n).wait_recv()
                row_hop(a, 1, n).start()
                row_hop(a, 2, n).start()

        @pl.when((n >= 1) & (n < n_ep + 1))
        def _():
            k = n - 1
            for a in range(2):
                shard_hop(a, 1, k).wait_recv()
                shard_hop(a, 3, k).start()

        @pl.when((n >= 2) & (n < n_ep + 1))
        def _():
            k = n - 1
            for a in range(2):
                row_hop(a, 1, k).wait_recv()
                row_hop(a, 3, k).start()

        @pl.when(n >= 3)
        def _():
            k = n - 2
            w_hop(k).wait_recv()
            for a in range(2):
                for kind in (2, 3):
                    row_hop(a, kind, k).wait_recv()

        @pl.when((n == 0) | (n >= 3))
        def _():
            compute(behind(jnp.maximum(n - 2, 0)))

    @pl.loop(0, n_ep)
    def _(k):
        for a in range(2):
            for kind in (2, 3):
                shard_hop(a, kind, k).wait_recv()
            for kind in (1, 2, 3):
                shard_hop(a, kind, k).wait_send()

    @pl.loop(1, n_ep)
    def _(k):
        for a in range(2):
            shard_hop(a, 0, k).wait_send()
            for kind in range(4):
                row_hop(a, kind, k).wait_send()
        w_hop(k).wait_send()

    for c in outs:
        c.wait()


def return_kernel(
    n_ep,
    n_tp,
    part,
    grad_in,
    grad_out,
    grad_gate,
    weight_part,
    rows_back,
    in_back,
    out_back,
    gate_back,
    weight_back,
    from_core,
    to_x,
    from_x,
    to_ep,
    send_core,
    recv_core,
    send_x,
    recv_x,
    send_ep,
    recv_ep,
    send_grad,
    recv_grad,
    send_w,
    recv_w,
):
    me = lax.axis_index("ep")
    t = lax.axis_index("tp")
    half = t // 2
    side = t % 2
    t_core = half * 2 + 1 - side
    t_x = (1 - half) * 2 + side
    cols = rows_back.shape[2]

    def ahead(k):
        return lax.rem(me + k, n_ep)

    def quarter(q):
        return pl.ds(pl.multiple_of(q * cols, cols), cols)

    core_peer = (me, t_core)
    x_peer = (me, t_x)
    others = [
        (ahead(k), lax.rem(t + d, n_tp))
        for k in range(n_ep)
        for d in range(n_tp)
        if k > 0 or d > 0
    ]
    greet(others)

    def copy_to(src, dst, send, recv, device):
        return pltpu.make_async_remote_copy(
            src_ref=src,
            dst_ref=dst,
            send_sem=send,
            recv_sem=recv,
            device_id=device,
            device_id_type=MESH,
        )

    started = []

    def go(copy):
        copy.start()
        started.append(copy)

    order = list(range(1, n_ep)) + [0]

    def core_hop(k, h):
        j = ahead(k)
        return copy_to(
            part.at[j, :, quarter(h * 2 + 1 - side)],
            from_core.at[k, h],
            send_core.at[k, h],
            recv_core.at[k, h],
            core_peer,
        )

    def x_hop(k):
        return copy_to(to_x.at[k], from_x.at[k], send_x.at[k], recv_x.at[k], x_peer)

    def ep_hop(k):
        return copy_to(
            to_ep.at[k], rows_back.at[me], send_ep.at[k], recv_ep.at[k], (ahead(k), t)
        )

    for k in order:
        for h in range(2):
            go(core_hop(k, h))
    grads = ((grad_in, in_back), (grad_out, out_back), (grad_gate, gate_back))

    def grad_hop(a, k):
        src, dst = grads[a]
        return copy_to(
            src.at[ahead(k)],
            dst.at[me],
            send_grad.at[a, k],
            recv_grad.at[a, k],
            (ahead(k), t),
        )

    def w_hop(k, d):
        return copy_to(
            weight_part.at[ahead(k)],
            weight_back.at[me, t],
            send_w.at[k, d],
            recv_w.at[k, d],
            (ahead(k), lax.rem(t + d, n_tp)),
        )

    for k in range(n_ep):
        for d in range(n_tp):
            if k > 0 or d > 0:
                go(w_hop(k, d))
        if k > 0:
            for a in range(3):
                go(grad_hop(a, k))
    for a in range(3):
        grads[a][1][pl.ds(me, 1)] = grads[a][0][pl.ds(me, 1)]
    weight_back[pl.ds(me, 1), pl.ds(t, 1)] = weight_part[pl.ds(me, 1)][:, None]

    def finish(k):
        j = ahead(k)
        x_hop(k).wait_recv()
        mine = part[j, :, quarter(t)].astype(jnp.float32)
        mine = mine + from_core[k, half].astype(jnp.float32)
        mine = (mine + from_x[k].astype(jnp.float32)).astype(jnp.bfloat16)
        if k > 0:
            to_ep[k] = mine
            go(ep_hop(k))
        else:
            rows_back[me] = mine

    lag = 2
    for n, k in enumerate(order):
        j = ahead(k)
        for h in range(2):
            core_hop(k, h).wait_recv()
        other = part[j, :, quarter(t_x)].astype(jnp.float32)
        other = other + from_core[k, 1 - half].astype(jnp.float32)
        to_x[k] = other.astype(jnp.bfloat16)
        go(x_hop(k))
        if n >= lag:
            finish(order[n - lag])
    for k in order[n_ep - lag :]:
        finish(k)

    for k in range(n_ep):
        if k > 0:
            ep_hop(k).wait_recv()
            for a in range(3):
                grad_hop(a, k).wait_recv()
        for d in range(n_tp):
            if k > 0 or d > 0:
                w_hop(k, d).wait_recv()
    for c in started:
        c.wait_send()


def dispatch(n_ep, n_tp, *args):
    x_quarter, _, x_own, _, weight_rows, in_own, _, gate_w, _, _ = args
    cap, cols = x_quarter.shape[1:]
    width = x_own.shape[1]
    hidden = gate_w.shape[1]
    lanes = weight_rows.shape[2]
    bf = jnp.bfloat16
    dma = pltpu.SemaphoreType.DMA
    rows = jax.ShapeDtypeStruct((n_ep, cap, width), bf)
    inner = jax.ShapeDtypeStruct((n_ep, cap, hidden), bf)
    shard = jax.ShapeDtypeStruct((n_ep, n_tp) + in_own.shape, bf)
    return pl.pallas_call(
        functools.partial(dispatch_kernel, n_ep),
        out_shape=(
            rows,
            rows,
            inner,
            inner,
            inner,
            rows,
            jax.ShapeDtypeStruct((n_ep, 8, lanes), jnp.float32),
            shard,
            shard,
        ),
        in_specs=[ANY, ANY, ANY, ANY, VMEM, ANY, ANY, VMEM, VMEM, VMEM],
        out_specs=(VMEM,) * 7 + (ANY, ANY),
        scratch_shapes=[
            pltpu.VMEM((n_ep, cap, width), bf),
            pltpu.VMEM(weight_rows.shape, bf),
            pltpu.VMEM((2,) + in_own.shape, bf),
            dma((6,)),
            dma((2, 4, n_ep)),
            dma((2, 4, n_ep)),
            dma((2, 4, n_ep)),
            dma((2, 4, n_ep)),
            dma((n_ep,)),
            dma((n_ep,)),
        ],
        compiler_params=pltpu.CompilerParams(
            collective_id=0, has_side_effects=True, vmem_limit_bytes=56 * 1024 * 1024
        ),
        name="dispatch",
    )(*args)


def give_back(n_ep, n_tp, *args):
    part, grad_in, grad_out, grad_gate, weight_part = args
    cap, width = part.shape[1:]
    cols = width // n_tp
    bf = jnp.bfloat16
    dma = pltpu.SemaphoreType.DMA
    same = lambda a: jax.ShapeDtypeStruct(a.shape, a.dtype)
    return pl.pallas_call(
        functools.partial(return_kernel, n_ep, n_tp),
        out_shape=(
            jax.ShapeDtypeStruct((n_ep, cap, cols), bf),
            same(grad_in),
            same(grad_out),
            same(grad_gate),
            jax.ShapeDtypeStruct((n_ep, n_tp) + weight_part.shape[1:], weight_part.dtype),
        ),
        in_specs=[VMEM] * 5,
        out_specs=(VMEM,) * 5,
        scratch_shapes=[
            pltpu.VMEM((n_ep, 2, cap, cols), bf),
            pltpu.VMEM((n_ep, cap, cols), bf),
            pltpu.VMEM((n_ep, cap, cols), bf),
            pltpu.VMEM((n_ep, cap, cols), bf),
            dma((n_ep, 2)),
            dma((n_ep, 2)),
            dma((n_ep,)),
            dma((n_ep,)),
            dma((n_ep,)),
            dma((n_ep,)),
            dma((3, n_ep)),
            dma((3, n_ep)),
            dma((n_ep, n_tp)),
            dma((n_ep, n_tp)),
        ],
        compiler_params=pltpu.CompilerParams(
            collective_id=1, has_side_effects=True, vmem_limit_bytes=40 * 1024 * 1024
        ),
        name="give_back",
    )(*args)


def shards(
    tokens,
    cotangent,
    route_ids,
    route_weights,
    w_gate,
    w_up,
    w_down,
    dense_in,
    dense_out,
    dense_gate,
):
    count_ep = lax.axis_size("ep")
    count_tp = lax.axis_size("tp")
    ep_index = lax.axis_index("ep")
    tp_index = lax.axis_index("tp")
    tok_dev, model_width = tokens.shape
    top_k = route_ids.shape[1]
    col_count = model_width // count_tp
    capacity = 2 * tok_dev * top_k // count_ep
    lanes = -(-capacity // 128) * 128
    slot_total = count_ep * capacity
    bf = jnp.bfloat16
    f32 = jnp.float32

    names = jnp.arange(count_ep, dtype=jnp.int32)
    chosen = route_ids[:, :, None] == names[None, None, :]
    member = jnp.any(chosen, axis=1).astype(bf)
    row = jnp.arange(tok_dev, dtype=jnp.int32)
    below = (row[None, :] < row[:, None]).astype(bf)
    rank = jnp.dot(below, member, preferred_element_type=f32)
    slot_index = jnp.sum(jnp.where(chosen, rank[:, None, :], 0.0), axis=2).astype(jnp.int32)
    target = route_ids * capacity + slot_index
    lane_target = route_ids * lanes + slot_index
    slots = jnp.arange(slot_total, dtype=jnp.int32)
    pick = slots[:, None] == target[:, 0][None, :]
    for k in range(1, top_k):
        pick = pick | (slots[:, None] == target[:, k][None, :])
    pick = pick.astype(bf)
    tok_part = lax.dynamic_slice_in_dim(tokens, tp_index * col_count, col_count, 1)
    cot_part = lax.dynamic_slice_in_dim(cotangent, tp_index * col_count, col_count, 1)
    quarter_shape = (count_ep, capacity, col_count)
    x_quarter = jnp.dot(pick, tok_part, preferred_element_type=bf).reshape(quarter_shape)
    dy_quarter = jnp.dot(pick, cot_part, preferred_element_type=bf).reshape(quarter_shape)
    pick_own = lax.dynamic_slice_in_dim(pick, ep_index * capacity, capacity, 0)
    x_own = jnp.dot(pick_own, tokens, preferred_element_type=bf)
    dy_own = jnp.dot(pick_own, cotangent, preferred_element_type=bf)
    lane_slots = jnp.arange(count_ep * lanes, dtype=jnp.int32)
    lane_hits = lane_target[:, :, None] == lane_slots[None, None, :]
    weight_rows = jnp.sum(
        jnp.where(lane_hits, route_weights.astype(f32)[:, :, None], 0.0), axis=(0, 1)
    ).astype(bf)
    weight_rows = jnp.broadcast_to(
        weight_rows.reshape(count_ep, 1, lanes), (count_ep, 16, lanes)
    )
    x_in, scaled_in, act, d_gate, d_up, part, weight_part, in_all, out_all = dispatch(
        count_ep,
        count_tp,
        x_quarter,
        dy_quarter,
        x_own,
        dy_own,
        weight_rows,
        dense_in,
        dense_out,
        w_gate[0],
        w_up[0],
        w_down[0],
    )
    in_whole = in_all.reshape(model_width, -1)
    out_whole = out_all.reshape(model_width, -1)
    x_slots = x_in.reshape(slot_total, model_width)
    scaled_cot = scaled_in.reshape(slot_total, model_width)
    contract_rows = (((0,), (0,)), ((), ()))
    contract_cols = (((1,), (1,)), ((), ()))
    act, d_gate, d_up = (a.reshape(slot_total, -1) for a in (act, d_gate, d_up))
    grad_gate = lax.dot_general(x_slots, d_gate, contract_rows, preferred_element_type=f32)
    grad_up = lax.dot_general(x_slots, d_up, contract_rows, preferred_element_type=f32)
    grad_down = lax.dot_general(act, scaled_cot, contract_rows, preferred_element_type=f32)

    dense_pre = jnp.dot(tokens, in_whole, preferred_element_type=f32)
    dense_act = jax.nn.silu(dense_pre).astype(bf)
    dense_val = lax.dot_general(dense_act, out_whole, contract_cols, preferred_element_type=f32)
    mix = jax.nn.sigmoid(jnp.dot(tokens, dense_gate, preferred_element_type=f32))
    cot_wide = cotangent.astype(f32)
    dense_scaled = (mix[:, None] * cot_wide).astype(bf)
    dense_back = jnp.dot(dense_scaled, out_whole, preferred_element_type=f32)
    sig_pre = jax.nn.sigmoid(dense_pre)
    dense_dpre = (dense_back * sig_pre * (1.0 + dense_pre * (1.0 - sig_pre))).astype(bf)
    dlogit = mix * (1.0 - mix) * jnp.sum(cot_wide * dense_val, axis=1)
    in_rows = lax.dynamic_slice_in_dim(in_whole, tp_index * col_count, col_count, 0)
    gate_cols = lax.dynamic_slice_in_dim(dense_gate, tp_index * col_count, col_count, 0)
    dense_dx = lax.dot_general(dense_dpre, in_rows, contract_cols, preferred_element_type=f32)
    dense_dx = dense_dx + dlogit[:, None] * gate_cols.astype(f32)[None, :]
    block_cols = model_width // (count_ep * count_tp)
    tokens_own = lax.dynamic_index_in_dim(
        tokens.reshape(tok_dev, count_ep, count_tp, block_cols), tp_index, 2, keepdims=False
    ).reshape(tok_dev, count_ep * block_cols)
    scaled_own = lax.dynamic_index_in_dim(
        dense_scaled.reshape(tok_dev, count_ep, count_tp, block_cols), tp_index, 2, keepdims=False
    ).reshape(tok_dev, count_ep * block_cols)
    in_partial = lax.dot_general(tokens_own, dense_dpre, contract_rows, preferred_element_type=f32)
    out_partial = lax.dot_general(scaled_own, dense_act, contract_rows, preferred_element_type=f32)
    gate_partial = jnp.sum(tokens_own.astype(f32) * dlogit[:, None], axis=0)
    gate_partial = jnp.pad(
        gate_partial.reshape(count_ep, 1, block_cols), ((0, 0), (0, 7), (0, -block_cols % 128))
    )

    rows_back, in_back, out_back, gate_back, weight_back = give_back(
        count_ep,
        count_tp,
        part,
        in_partial.astype(bf).reshape(count_ep, block_cols, -1),
        out_partial.astype(bf).reshape(count_ep, block_cols, -1),
        gate_partial,
        weight_part,
    )
    grad_dense_in = jnp.sum(in_back.astype(f32), axis=0)
    grad_dense_out = jnp.sum(out_back.astype(f32), axis=0)
    grad_dense_gate = jnp.sum(gate_back[:, 0, :block_cols], axis=0)
    expert_dx = lax.dot_general(
        pick, rows_back.reshape(slot_total, col_count), contract_rows, preferred_element_type=f32
    )
    grad_tokens = (dense_dx + expert_dx).astype(bf)
    weight_grad = jnp.sum(weight_back[:, :, 0, :], axis=1).reshape(-1)
    grad_route_weights = jnp.sum(
        jnp.where(lane_hits, weight_grad[None, None, :], 0.0), axis=2
    ).astype(bf)
    return (
        grad_tokens,
        grad_route_weights,
        grad_gate[None],
        grad_up[None],
        grad_down[None],
        grad_dense_in,
        grad_dense_out,
        grad_dense_gate,
    )


def solution(mesh):
    placed = (
        P("ep", None),
        P("ep", None),
        P("ep", None),
        P("ep", None),
        P("ep", None, "tp"),
        P("ep", None, "tp"),
        P("ep", "tp", None),
        P(("ep", "tp"), None),
        P(("ep", "tp"), None),
        P(),
    )
    return jax.shard_map(
        shards,
        mesh=mesh,
        in_specs=placed,
        out_specs=(
            P("ep", "tp"),
            P("ep", None),
            P("ep", None, "tp"),
            P("ep", None, "tp"),
            P("ep", "tp", None),
            P(("ep", "tp"), None),
            P(("ep", "tp"), None),
            P(("ep", "tp")),
        ),
        check_vma=False,
    )
```

```python
import functools

import jax
import jax.numpy as jnp
from jax import lax
from jax.experimental import pallas as pl
from jax.experimental.pallas import tpu as pltpu
from jax.sharding import PartitionSpec as P

CLAMP_LIMIT = 7.0
SIG_SLOPE = 1.702
MESH = pl.DeviceIdType.MESH
ANY = pl.BlockSpec(memory_space=pl.ANY)
VMEM = pl.BlockSpec(memory_space=pltpu.VMEM)


def greet(devices):
    barrier = pltpu.get_barrier_semaphore()
    for device in devices:
        pl.semaphore_signal(barrier, inc=1, device_id=device, device_id_type=MESH)
    pl.semaphore_wait(barrier, len(devices))


def dispatch_kernel(
    n_ep,
    x_quarter,
    dy_quarter,
    x_own,
    dy_own,
    weight_rows,
    in_own,
    out_own,
    gate_w,
    up_w,
    down_w,
    x_out,
    scaled_out,
    act_out,
    dgate_out,
    dup_out,
    part_out,
    weight_part,
    in_all,
    out_all,
    x_all,
    scaled_all,
    act_all,
    dgate_all,
    dup_all,
    part_all,
    dy_all,
    weight_all,
    shard_buf,
    local_sem,
    out_sem,
    send_rows,
    recv_rows,
    send_shard,
    recv_shard,
    send_w,
    recv_w,
):
    me = lax.axis_index("ep")
    t = lax.axis_index("tp")
    half = t // 2
    side = t % 2
    t_core = half * 2 + 1 - side
    t_x = (1 - half) * 2 + side
    cap, cols = x_quarter.shape[1:]
    lanes = weight_rows.shape[2]
    f32 = jnp.float32
    bf = jnp.bfloat16

    def ahead(k):
        return lax.rem(me + k, n_ep)

    def behind(k):
        return lax.rem(me + n_ep - k, n_ep)

    def offset(n):
        return n_ep // 2 + (n // 2) * (1 - 2 * (n % 2))

    core_peer = (me, t_core)
    x_peer = (me, t_x)
    greet([(ahead(k), t) for k in range(1, n_ep)] + [core_peer, x_peer])

    rows_in = (x_quarter, dy_quarter)
    rows_out = (x_all, dy_all)
    shards_in = (in_own, out_own)
    shards_out = (in_all, out_all)

    def row_slice(a, i, q):
        return rows_out[a].at[i, :, pl.ds(pl.multiple_of(q * cols, cols), cols)]

    def copy_to(src, dst, send, recv, device):
        return pltpu.make_async_remote_copy(
            src_ref=src,
            dst_ref=dst,
            send_sem=send,
            recv_sem=recv,
            device_id=device,
            device_id_type=MESH,
        )

    def shard_hop(a, kind, k, first=False):
        i = behind(k)
        sems = (send_shard.at[a, kind, k], recv_shard.at[a, kind, k])
        if kind == 0:
            return copy_to(shards_in[a], shards_out[a].at[me, t], *sems, (ahead(k), t))
        if kind == 3:
            block = shards_out[a].at[i, t_x]
            return copy_to(block, block, *sems, core_peer)
        block = shards_out[a].at[i, t]
        return copy_to(
            shards_in[a] if first else block, block, *sems, x_peer if kind == 1 else core_peer
        )

    def row_hop(a, kind, k):
        i = behind(k)
        sems = (send_rows.at[a, kind, k], recv_rows.at[a, kind, k])
        if kind == 0:
            return copy_to(rows_in[a].at[ahead(k)], row_slice(a, me, t), *sems, (ahead(k), t))
        block = row_slice(a, i, t_x if kind == 3 else t)
        return copy_to(block, block, *sems, x_peer if kind == 1 else core_peer)

    def w_hop(k):
        return copy_to(
            weight_rows.at[ahead(k)], weight_all.at[me], send_w.at[k], recv_w.at[k], (ahead(k), t)
        )

    for a in range(2):
        shard_hop(a, 1, 0, True).start()
        shard_hop(a, 2, 0, True).start()

    @pl.loop(1, n_ep)
    def _(n):
        k = offset(n)
        for a in range(2):
            shard_hop(a, 0, k).start()
        w_hop(k).start()
        for a in range(2):
            row_hop(a, 0, k).start()

    ins = [
        pltpu.make_async_copy(in_own, shard_buf.at[0], local_sem.at[0]),
        pltpu.make_async_copy(out_own, shard_buf.at[1], local_sem.at[1]),
        pltpu.make_async_copy(x_own, x_all.at[me], local_sem.at[2]),
        pltpu.make_async_copy(dy_own, dy_all.at[me], local_sem.at[3]),
    ]
    outs = [
        pltpu.make_async_copy(shard_buf.at[0], in_all.at[me, t], local_sem.at[4]),
        pltpu.make_async_copy(shard_buf.at[1], out_all.at[me, t], local_sem.at[5]),
    ]
    for c in ins:
        c.start()
    weight_all[pl.ds(me, 1)] = weight_rows[pl.ds(me, 1)]
    for c in ins:
        c.wait()
    for c in outs:
        c.start()

    diagonal = lax.broadcasted_iota(jnp.int32, (cap, lanes), 0) == lax.broadcasted_iota(
        jnp.int32, (cap, lanes), 1
    )
    contract_cols = (((1,), (1,)), ((), ()))

    def compute(i):
        weight_row = weight_all[i, 0:1].astype(f32)
        route_col = jnp.sum(jnp.where(diagonal, weight_row, 0.0), axis=1, keepdims=True)
        x_rows = x_all[i]
        gate_pre = jnp.dot(x_rows, gate_w[...], preferred_element_type=f32)
        up_pre = jnp.dot(x_rows, up_w[...], preferred_element_type=f32)
        gate_clamp = jnp.minimum(gate_pre, CLAMP_LIMIT)
        up_clamp = jnp.clip(up_pre, -CLAMP_LIMIT, CLAMP_LIMIT)
        sig = jax.nn.sigmoid(SIG_SLOPE * gate_clamp)
        act = (gate_clamp * sig * (up_clamp + 1.0)).astype(bf)
        act_all[i] = act
        dy_rows = dy_all[i]
        scaled_all[i] = (route_col * dy_rows.astype(f32)).astype(bf)
        back = lax.dot_general(
            dy_rows, down_w[...], contract_cols, preferred_element_type=f32
        )
        weight_sum = jnp.sum(act.astype(f32) * back, axis=1, keepdims=True)
        weight_lane = jnp.sum(jnp.where(diagonal, weight_sum, 0.0), axis=0, keepdims=True)
        weight_part[i] = jnp.broadcast_to(weight_lane, (8, lanes))
        d_act = route_col * back
        d_gate = jnp.where(
            gate_pre < CLAMP_LIMIT,
            d_act * (up_clamp + 1.0) * (sig + SIG_SLOPE * gate_clamp * sig * (1.0 - sig)),
            0.0,
        ).astype(bf)
        d_up = jnp.where(jnp.abs(up_pre) < CLAMP_LIMIT, d_act * gate_clamp * sig, 0.0).astype(bf)
        dgate_all[i] = d_gate
        dup_all[i] = d_up
        part = lax.dot_general(d_gate, gate_w[...], contract_cols, preferred_element_type=f32)
        part = part + lax.dot_general(d_up, up_w[...], contract_cols, preferred_element_type=f32)
        part_all[i] = part.astype(bf)

    results = (
        (x_all, x_out),
        (part_all, part_out),
        (scaled_all, scaled_out),
        (act_all, act_out),
        (dgate_all, dgate_out),
        (dup_all, dup_out),
    )

    def store(i):
        return [
            pltpu.make_async_copy(src.at[i], dst.at[i], out_sem.at[a, i])
            for a, (src, dst) in enumerate(results)
        ]

    @pl.loop(0, n_ep + 2)
    def _(n):
        @pl.when((n >= 1) & (n < n_ep))
        def _():
            k = offset(n)
            for a in range(2):
                shard_hop(a, 0, k).wait_recv()
                shard_hop(a, 1, k).start()
                shard_hop(a, 2, k).start()
            for a in range(2):
                row_hop(a, 0, k).wait_recv()
                row_hop(a, 1, k).start()
                row_hop(a, 2, k).start()

        @pl.when((n >= 1) & (n < n_ep + 1))
        def _():
            k = jnp.where(n == 1, 0, offset(jnp.maximum(n - 1, 1)))
            for a in range(2):
                shard_hop(a, 1, k).wait_recv()
                shard_hop(a, 3, k).start()

        @pl.when((n >= 2) & (n < n_ep + 1))
        def _():
            k = offset(n - 1)
            for a in range(2):
                row_hop(a, 1, k).wait_recv()
                row_hop(a, 3, k).start()

        @pl.when(n >= 3)
        def _():
            k = offset(n - 2)
            w_hop(k).wait_recv()
            for a in range(2):
                for kind in (2, 3):
                    row_hop(a, kind, k).wait_recv()

        @pl.when((n == 0) | (n >= 3))
        def _():
            i = behind(jnp.where(n == 0, 0, offset(jnp.maximum(n - 2, 1))))
            compute(i)
            for c in store(i):
                c.start()

    @pl.loop(0, n_ep)
    def _(k):
        for a in range(2):
            for kind in (2, 3):
                shard_hop(a, kind, k).wait_recv()
            for kind in (1, 2, 3):
                shard_hop(a, kind, k).wait_send()
        for c in store(k):
            c.wait()

    @pl.loop(1, n_ep)
    def _(k):
        for a in range(2):
            shard_hop(a, 0, k).wait_send()
            for kind in range(4):
                row_hop(a, kind, k).wait_send()
        w_hop(k).wait_send()

    for c in outs:
        c.wait()


def return_kernel(
    n_ep,
    n_tp,
    part,
    grad_in,
    grad_out,
    grad_gate,
    weight_part,
    rows_back,
    in_back,
    out_back,
    gate_back,
    weight_back,
    from_core,
    to_x,
    from_x,
    to_ep,
    send_core,
    recv_core,
    send_x,
    recv_x,
    send_ep,
    recv_ep,
    send_grad,
    recv_grad,
    send_w,
    recv_w,
):
    me = lax.axis_index("ep")
    t = lax.axis_index("tp")
    half = t // 2
    side = t % 2
    t_core = half * 2 + 1 - side
    t_x = (1 - half) * 2 + side
    cols = rows_back.shape[2]

    def ahead(k):
        return lax.rem(me + k, n_ep)

    def quarter(q):
        return pl.ds(pl.multiple_of(q * cols, cols), cols)

    core_peer = (me, t_core)
    x_peer = (me, t_x)
    others = [
        (ahead(k), lax.rem(t + d, n_tp))
        for k in range(n_ep)
        for d in range(n_tp)
        if k > 0 or d > 0
    ]
    greet(others)

    def copy_to(src, dst, send, recv, device):
        return pltpu.make_async_remote_copy(
            src_ref=src,
            dst_ref=dst,
            send_sem=send,
            recv_sem=recv,
            device_id=device,
            device_id_type=MESH,
        )

    started = []

    def go(copy):
        copy.start()
        started.append(copy)

    order = list(range(1, n_ep)) + [0]

    def core_hop(k, h):
        j = ahead(k)
        return copy_to(
            part.at[j, :, quarter(h * 2 + 1 - side)],
            from_core.at[k, h],
            send_core.at[k, h],
            recv_core.at[k, h],
            core_peer,
        )

    def x_hop(k):
        return copy_to(to_x.at[k], from_x.at[k], send_x.at[k], recv_x.at[k], x_peer)

    def ep_hop(k):
        return copy_to(
            to_ep.at[k], rows_back.at[me], send_ep.at[k], recv_ep.at[k], (ahead(k), t)
        )

    for k in order:
        for h in range(2):
            go(core_hop(k, h))
    grads = ((grad_in, in_back), (grad_out, out_back), (grad_gate, gate_back))

    def grad_hop(a, k):
        src, dst = grads[a]
        return copy_to(
            src.at[ahead(k)],
            dst.at[me],
            send_grad.at[a, k],
            recv_grad.at[a, k],
            (ahead(k), t),
        )

    def w_hop(k, d):
        return copy_to(
            weight_part.at[ahead(k)],
            weight_back.at[me, t],
            send_w.at[k, d],
            recv_w.at[k, d],
            (ahead(k), lax.rem(t + d, n_tp)),
        )

    for k in range(n_ep):
        for d in range(n_tp):
            if k > 0 or d > 0:
                go(w_hop(k, d))
        if k > 0:
            for a in range(3):
                go(grad_hop(a, k))
    for a in range(3):
        grads[a][1][pl.ds(me, 1)] = grads[a][0][pl.ds(me, 1)]
    weight_back[pl.ds(me, 1), pl.ds(t, 1)] = weight_part[pl.ds(me, 1)][:, None]

    def finish(k):
        j = ahead(k)
        x_hop(k).wait_recv()
        mine = part[j, :, quarter(t)].astype(jnp.float32)
        mine = mine + from_core[k, half].astype(jnp.float32)
        mine = (mine + from_x[k].astype(jnp.float32)).astype(jnp.bfloat16)
        if k > 0:
            to_ep[k] = mine
            go(ep_hop(k))
        else:
            rows_back[me] = mine

    lag = 2
    for n, k in enumerate(order):
        j = ahead(k)
        for h in range(2):
            core_hop(k, h).wait_recv()
        other = part[j, :, quarter(t_x)].astype(jnp.float32)
        other = other + from_core[k, 1 - half].astype(jnp.float32)
        to_x[k] = other.astype(jnp.bfloat16)
        go(x_hop(k))
        if n >= lag:
            finish(order[n - lag])
    for k in order[n_ep - lag :]:
        finish(k)

    for k in range(n_ep):
        if k > 0:
            ep_hop(k).wait_recv()
            for a in range(3):
                grad_hop(a, k).wait_recv()
        for d in range(n_tp):
            if k > 0 or d > 0:
                w_hop(k, d).wait_recv()
    for c in started:
        c.wait_send()


def dispatch(n_ep, n_tp, *args):
    x_quarter, _, x_own, _, weight_rows, in_own, _, gate_w, _, _ = args
    cap, cols = x_quarter.shape[1:]
    width = x_own.shape[1]
    hidden = gate_w.shape[1]
    lanes = weight_rows.shape[2]
    bf = jnp.bfloat16
    dma = pltpu.SemaphoreType.DMA
    rows = jax.ShapeDtypeStruct((n_ep, cap, width), bf)
    inner = jax.ShapeDtypeStruct((n_ep, cap, hidden), bf)
    shard = jax.ShapeDtypeStruct((n_ep, n_tp) + in_own.shape, bf)
    return pl.pallas_call(
        functools.partial(dispatch_kernel, n_ep),
        out_shape=(
            rows,
            rows,
            inner,
            inner,
            inner,
            rows,
            jax.ShapeDtypeStruct((n_ep, 8, lanes), jnp.float32),
            shard,
            shard,
        ),
        in_specs=[ANY, ANY, ANY, ANY, VMEM, ANY, ANY, VMEM, VMEM, VMEM],
        out_specs=(ANY,) * 6 + (VMEM, ANY, ANY),
        scratch_shapes=[
            pltpu.VMEM(rows.shape, bf),
            pltpu.VMEM(rows.shape, bf),
            pltpu.VMEM(inner.shape, bf),
            pltpu.VMEM(inner.shape, bf),
            pltpu.VMEM(inner.shape, bf),
            pltpu.VMEM(rows.shape, bf),
            pltpu.VMEM(rows.shape, bf),
            pltpu.VMEM(weight_rows.shape, bf),
            pltpu.VMEM((2,) + in_own.shape, bf),
            dma((6,)),
            dma((6, n_ep)),
            dma((2, 4, n_ep)),
            dma((2, 4, n_ep)),
            dma((2, 4, n_ep)),
            dma((2, 4, n_ep)),
            dma((n_ep,)),
            dma((n_ep,)),
        ],
        compiler_params=pltpu.CompilerParams(
            collective_id=0, has_side_effects=True, vmem_limit_bytes=56 * 1024 * 1024
        ),
        name="dispatch",
    )(*args)


def give_back(n_ep, n_tp, *args):
    part, grad_in, grad_out, grad_gate, weight_part = args
    cap, width = part.shape[1:]
    cols = width // n_tp
    bf = jnp.bfloat16
    dma = pltpu.SemaphoreType.DMA
    same = lambda a: jax.ShapeDtypeStruct(a.shape, a.dtype)
    return pl.pallas_call(
        functools.partial(return_kernel, n_ep, n_tp),
        out_shape=(
            jax.ShapeDtypeStruct((n_ep, cap, cols), bf),
            same(grad_in),
            same(grad_out),
            same(grad_gate),
            jax.ShapeDtypeStruct((n_ep, n_tp) + weight_part.shape[1:], weight_part.dtype),
        ),
        in_specs=[VMEM] * 5,
        out_specs=(VMEM,) * 5,
        scratch_shapes=[
            pltpu.VMEM((n_ep, 2, cap, cols), bf),
            pltpu.VMEM((n_ep, cap, cols), bf),
            pltpu.VMEM((n_ep, cap, cols), bf),
            pltpu.VMEM((n_ep, cap, cols), bf),
            dma((n_ep, 2)),
            dma((n_ep, 2)),
            dma((n_ep,)),
            dma((n_ep,)),
            dma((n_ep,)),
            dma((n_ep,)),
            dma((3, n_ep)),
            dma((3, n_ep)),
            dma((n_ep, n_tp)),
            dma((n_ep, n_tp)),
        ],
        compiler_params=pltpu.CompilerParams(
            collective_id=1, has_side_effects=True, vmem_limit_bytes=40 * 1024 * 1024
        ),
        name="give_back",
    )(*args)


def shards(
    tokens,
    cotangent,
    route_ids,
    route_weights,
    w_gate,
    w_up,
    w_down,
    dense_in,
    dense_out,
    dense_gate,
):
    count_ep = lax.axis_size("ep")
    count_tp = lax.axis_size("tp")
    ep_index = lax.axis_index("ep")
    tp_index = lax.axis_index("tp")
    tok_dev, model_width = tokens.shape
    top_k = route_ids.shape[1]
    col_count = model_width // count_tp
    capacity = 2 * tok_dev * top_k // count_ep
    lanes = -(-capacity // 128) * 128
    slot_total = count_ep * capacity
    bf = jnp.bfloat16
    f32 = jnp.float32

    names = jnp.arange(count_ep, dtype=jnp.int32)
    chosen = route_ids[:, :, None] == names[None, None, :]
    member = jnp.any(chosen, axis=1).astype(bf)
    row = jnp.arange(tok_dev, dtype=jnp.int32)
    below = (row[None, :] < row[:, None]).astype(bf)
    rank = jnp.dot(below, member, preferred_element_type=f32)
    slot_index = jnp.sum(jnp.where(chosen, rank[:, None, :], 0.0), axis=2).astype(jnp.int32)
    target = route_ids * capacity + slot_index
    lane_target = route_ids * lanes + slot_index
    slots = jnp.arange(slot_total, dtype=jnp.int32)
    pick = slots[:, None] == target[:, 0][None, :]
    for k in range(1, top_k):
        pick = pick | (slots[:, None] == target[:, k][None, :])
    pick = pick.astype(bf)
    tok_part = lax.dynamic_slice_in_dim(tokens, tp_index * col_count, col_count, 1)
    cot_part = lax.dynamic_slice_in_dim(cotangent, tp_index * col_count, col_count, 1)
    quarter_shape = (count_ep, capacity, col_count)
    x_quarter = jnp.dot(pick, tok_part, preferred_element_type=bf).reshape(quarter_shape)
    dy_quarter = jnp.dot(pick, cot_part, preferred_element_type=bf).reshape(quarter_shape)
    pick_own = lax.dynamic_slice_in_dim(pick, ep_index * capacity, capacity, 0)
    x_own = jnp.dot(pick_own, tokens, preferred_element_type=bf)
    dy_own = jnp.dot(pick_own, cotangent, preferred_element_type=bf)
    lane_slots = jnp.arange(count_ep * lanes, dtype=jnp.int32)
    lane_hits = lane_target[:, :, None] == lane_slots[None, None, :]
    weight_rows = jnp.sum(
        jnp.where(lane_hits, route_weights.astype(f32)[:, :, None], 0.0), axis=(0, 1)
    ).astype(bf)
    weight_rows = jnp.broadcast_to(
        weight_rows.reshape(count_ep, 1, lanes), (count_ep, 16, lanes)
    )
    x_in, scaled_in, act, d_gate, d_up, part, weight_part, in_all, out_all = dispatch(
        count_ep,
        count_tp,
        x_quarter,
        dy_quarter,
        x_own,
        dy_own,
        weight_rows,
        dense_in,
        dense_out,
        w_gate[0],
        w_up[0],
        w_down[0],
    )
    in_whole = in_all.reshape(model_width, -1)
    out_whole = out_all.reshape(model_width, -1)
    x_slots = x_in.reshape(slot_total, model_width)
    scaled_cot = scaled_in.reshape(slot_total, model_width)
    contract_rows = (((0,), (0,)), ((), ()))
    contract_cols = (((1,), (1,)), ((), ()))
    act, d_gate, d_up = (a.reshape(slot_total, -1) for a in (act, d_gate, d_up))
    grad_gate = lax.dot_general(x_slots, d_gate, contract_rows, preferred_element_type=f32)
    grad_up = lax.dot_general(x_slots, d_up, contract_rows, preferred_element_type=f32)
    grad_down = lax.dot_general(act, scaled_cot, contract_rows, preferred_element_type=f32)

    dense_pre = jnp.dot(tokens, in_whole, preferred_element_type=f32)
    dense_act = jax.nn.silu(dense_pre).astype(bf)
    dense_val = lax.dot_general(dense_act, out_whole, contract_cols, preferred_element_type=f32)
    mix = jax.nn.sigmoid(jnp.dot(tokens, dense_gate, preferred_element_type=f32))
    cot_wide = cotangent.astype(f32)
    dense_scaled = (mix[:, None] * cot_wide).astype(bf)
    dense_back = jnp.dot(dense_scaled, out_whole, preferred_element_type=f32)
    sig_pre = jax.nn.sigmoid(dense_pre)
    dense_dpre = (dense_back * sig_pre * (1.0 + dense_pre * (1.0 - sig_pre))).astype(bf)
    dlogit = mix * (1.0 - mix) * jnp.sum(cot_wide * dense_val, axis=1)
    in_rows = lax.dynamic_slice_in_dim(in_whole, tp_index * col_count, col_count, 0)
    gate_cols = lax.dynamic_slice_in_dim(dense_gate, tp_index * col_count, col_count, 0)
    dense_dx = lax.dot_general(dense_dpre, in_rows, contract_cols, preferred_element_type=f32)
    dense_dx = dense_dx + dlogit[:, None] * gate_cols.astype(f32)[None, :]
    block_cols = model_width // (count_ep * count_tp)
    tokens_own = lax.dynamic_index_in_dim(
        tokens.reshape(tok_dev, count_ep, count_tp, block_cols), tp_index, 2, keepdims=False
    ).reshape(tok_dev, count_ep * block_cols)
    scaled_own = lax.dynamic_index_in_dim(
        dense_scaled.reshape(tok_dev, count_ep, count_tp, block_cols), tp_index, 2, keepdims=False
    ).reshape(tok_dev, count_ep * block_cols)
    in_partial = lax.dot_general(tokens_own, dense_dpre, contract_rows, preferred_element_type=f32)
    out_partial = lax.dot_general(scaled_own, dense_act, contract_rows, preferred_element_type=f32)
    gate_partial = jnp.sum(tokens_own.astype(f32) * dlogit[:, None], axis=0)
    gate_partial = jnp.pad(
        gate_partial.reshape(count_ep, 1, block_cols), ((0, 0), (0, 7), (0, -block_cols % 128))
    )

    rows_back, in_back, out_back, gate_back, weight_back = give_back(
        count_ep,
        count_tp,
        part,
        in_partial.astype(bf).reshape(count_ep, block_cols, -1),
        out_partial.astype(bf).reshape(count_ep, block_cols, -1),
        gate_partial,
        weight_part,
    )
    grad_dense_in = jnp.sum(in_back.astype(f32), axis=0)
    grad_dense_out = jnp.sum(out_back.astype(f32), axis=0)
    grad_dense_gate = jnp.sum(gate_back[:, 0, :block_cols], axis=0)
    expert_dx = lax.dot_general(
        pick, rows_back.reshape(slot_total, col_count), contract_rows, preferred_element_type=f32
    )
    grad_tokens = (dense_dx + expert_dx).astype(bf)
    weight_grad = jnp.sum(weight_back[:, :, 0, :], axis=1).reshape(-1)
    grad_route_weights = jnp.sum(
        jnp.where(lane_hits, weight_grad[None, None, :], 0.0), axis=2
    ).astype(bf)
    return (
        grad_tokens,
        grad_route_weights,
        grad_gate[None],
        grad_up[None],
        grad_down[None],
        grad_dense_in,
        grad_dense_out,
        grad_dense_gate,
    )


def solution(mesh):
    placed = (
        P("ep", None),
        P("ep", None),
        P("ep", None),
        P("ep", None),
        P("ep", None, "tp"),
        P("ep", None, "tp"),
        P("ep", "tp", None),
        P(("ep", "tp"), None),
        P(("ep", "tp"), None),
        P(),
    )
    return jax.shard_map(
        shards,
        mesh=mesh,
        in_specs=placed,
        out_specs=(
            P("ep", "tp"),
            P("ep", None),
            P("ep", None, "tp"),
            P("ep", None, "tp"),
            P("ep", "tp", None),
            P(("ep", "tp"), None),
            P(("ep", "tp"), None),
            P(("ep", "tp")),
        ),
        check_vma=False,
    )
```
